32 devices in a mesh: rep: 4 (over z), fs: 4 (over y, x), tp: 2 (over core).
Axes of the slice: x: 2, y: 2, z: 4, core: 2. Of those that a mesh axis runs over, the one named last changes fastest.
Arguments:
- inputs: bfloat16 [4, 1024, 1024], P('rep', ('fs', 'tp')), may hold values from -6 to 6
- up_pre: bfloat16 [4, 1024, 2816], P('rep', None, ('fs', 'tp')), may hold values from -6 to 6
- gate_pre: bfloat16 [4, 1024, 2816], P('rep', None, ('fs', 'tp')), may hold values from -6 to 6
- cotangent: bfloat16 [4, 1024, 1024], P('rep', ('fs', 'tp')), may hold values from -6 to 6
- w_up: float32 [1024, 2816], P(None, ('fs', 'tp')), may hold values from -0.1875 to 0.1875
- w_gate: float32 [1024, 2816], P(None, ('fs', 'tp')), may hold values from -0.1875 to 0.1875
- w_down: float32 [2816, 1024], P(('fs', 'tp')), may hold values from -0.109375 to 0.109375
- conv_weight: float32 [3, 2816], P(None, ('fs', 'tp')), may hold values from -3.5 to 3.5
- conv_bias: float32 [2816], P(('fs', 'tp')), may hold values from -3 to 3
Outputs:
- grad_inputs: bfloat16 [4, 1024, 1024], P('rep', ('fs', 'tp'))
- grad_up: float32 [1024, 2816], P(None, ('fs', 'tp'))
- grad_gate: float32 [1024, 2816], P(None, ('fs', 'tp'))
- grad_down: float32 [2816, 1024], P(('fs', 'tp'))
- grad_conv_weight: float32 [3, 2816], P(None, ('fs', 'tp'))
- grad_conv_bias: float32 [2816], P(('fs', 'tp'))
The draws below stay inside these ranges and needn't reach their ends.
All inputs are finite; a program needn't handle non-finite values.
Results may differ from the reference program's by a relative error of at most 0.0085.
Values may be sent and summed in bfloat16 or wider, within the bound.
A program may use at most 64 MiB of HBM per device.

```python
import jax
import jax.numpy as jnp
from jax import lax

D = 1024
FF = 2816
CONV = 3
SEQ = 1024
BATCH = 4


def raised(values, rng, source, target, blocks, factor):
    def block_of(dim):
        return (jnp.arange(values.shape[dim]) // (values.shape[dim] // blocks)).reshape((-1,) + (1,) * (values.ndim - 1 - dim))

    near = jax.random.permutation(rng, blocks)[block_of(target)]
    other_side = (block_of(target) + blocks // 2) % blocks
    return jnp.where((block_of(source) == near) | (block_of(source) == other_side), factor * values, values)


def level_of(rng, extent, shards, least, top_value):
    loudness = 1.0
    for axis_at, blocks in shards:
        steps = jax.random.uniform(jax.random.fold_in(jax.random.fold_in(rng, 6), axis_at), (blocks,), jnp.float32, least / len(shards), top_value / len(shards))
        loudness = loudness * jnp.repeat(jnp.exp(steps), extent[axis_at] // blocks).reshape((-1,) + (1,) * (len(extent) - 1 - axis_at))
    return loudness


def scatter_about(key, dims, scale, most, pieces=(), held_as=jnp.bfloat16):
    entries = scale * jax.random.normal(key, dims, jnp.float32)
    if pieces:
        entries = entries * level_of(key, dims, pieces, -0.22, 0.18)
    return jnp.clip(entries, -most, most).astype(held_as)


def bell_draw_with(key, extent, deviation, reach, shards, heavy, held_as=jnp.bfloat16):
    values = deviation * jax.random.normal(key, extent, jnp.float32)
    if shards:
        values = values * level_of(key, extent, shards, -0.22, 0.18)
    return jnp.clip(raised(values, jax.random.fold_in(key, 3), *heavy), -reach, reach).astype(held_as)


def setup_inputs(seed: int = 0) -> dict:
    streams_of = jax.random.split(jax.random.key(seed), 10)
    return {
        "inputs": scatter_about(streams_of[0], (BATCH, SEQ, D), 1.0, 6.0, ((0, 4), (1, 8))),
        "up_pre": scatter_about(streams_of[1], (BATCH, SEQ, FF), 1.0, 6.0, ((0, 4), (2, 8))),
        "gate_pre": scatter_about(streams_of[2], (BATCH, SEQ, FF), 1.0, 6.0, ((0, 4), (2, 8))),
        "cotangent": bell_draw_with(streams_of[3], (BATCH, SEQ, D), 1.0, 6.0, ((0, 4), (1, 8)), (0, 2, 4, 2.0)),
        "w_up": scatter_about(streams_of[4], (D, FF), D ** -0.5, 0.1875, ((1, 8),), jnp.float32),
        "w_gate": scatter_about(streams_of[5], (D, FF), D ** -0.5, 0.1875, ((1, 8),), jnp.float32),
        "w_down": scatter_about(streams_of[6], (FF, D), FF ** -0.5, 0.109375, ((0, 8),), jnp.float32),
        "conv_weight": scatter_about(streams_of[7], (CONV, FF), CONV ** -0.5, 3.5, ((1, 8),), jnp.float32),
        "conv_bias": scatter_about(streams_of[8], (FF,), 0.5, 3.0, ((0, 8),), jnp.float32),
    }


def conv_forward(up_rows, conv_weight, conv_bias):
    length = up_rows.shape[0]
    tap_count = conv_weight.shape[0]
    padded = jnp.pad(up_rows, ((tap_count - 1, 0), (0, 0)))
    result = conv_bias + jnp.zeros_like(up_rows)
    for tap_index in range(tap_count):
        begin = tap_count - 1 - tap_index
        result = result + conv_weight[tap_index] * padded[begin:begin + length]
    return result

def conv_back(d_conv, up_rows, conv_weight):
    length = up_rows.shape[0]
    tap_count = conv_weight.shape[0]
    padded_grad = jnp.pad(d_conv, ((0, tap_count - 1), (0, 0)))
    padded_up = jnp.pad(up_rows, ((tap_count - 1, 0), (0, 0)))
    d_up = jnp.zeros_like(d_conv)
    tap_grads = []
    for tap_index in range(tap_count):
        d_up = d_up + conv_weight[tap_index] * padded_grad[tap_index:tap_index + length]
        begin = tap_count - 1 - tap_index
        tap_grads.append(lax.optimization_barrier(jnp.sum(d_conv * padded_up[begin:begin + length], axis=0)))
    return (d_up, jnp.stack(tap_grads), lax.optimization_barrier(jnp.sum(d_conv, axis=0)))

def reference(inputs, up_pre, gate_pre, cotangent, w_up, w_gate, w_down, conv_weight, conv_bias):
    up_mat = w_up.astype(jnp.bfloat16)
    gate_mat = w_gate.astype(jnp.bfloat16)
    down_mat = w_down.astype(jnp.bfloat16)

    def one_sequence(running, sequence):
        seq_inputs, seq_up, seq_gate, seq_cot = sequence
        up_rows = seq_up.astype(jnp.float32)
        gate_rows = seq_gate.astype(jnp.float32)
        convolved = conv_forward(up_rows, conv_weight, conv_bias)
        activated, pullback = jax.vjp(jax.nn.gelu, convolved)
        hidden = (activated * gate_rows).astype(jnp.bfloat16)
        d_hidden = jnp.dot(seq_cot, down_mat.T, preferred_element_type=jnp.float32).astype(jnp.bfloat16)
        d_hidden_f = d_hidden.astype(jnp.float32)
        d_gate = (d_hidden_f * activated).astype(jnp.bfloat16)
        d_conv = pullback(d_hidden_f * gate_rows)[0]
        d_up_f, tap_grad, bias_grad = conv_back(d_conv, up_rows, conv_weight)
        d_up = d_up_f.astype(jnp.bfloat16)
        grad_rows = (jnp.dot(d_up, up_mat.T, preferred_element_type=jnp.float32) + jnp.dot(d_gate, gate_mat.T, preferred_element_type=jnp.float32)).astype(jnp.bfloat16)
        g_up = jnp.dot(seq_inputs.T, d_up, preferred_element_type=jnp.float32)
        g_gate = jnp.dot(seq_inputs.T, d_gate, preferred_element_type=jnp.float32)
        g_down = jnp.dot(hidden.T, seq_cot, preferred_element_type=jnp.float32)
        updated = (running[0] + g_up, running[1] + g_gate, running[2] + g_down, running[3] + tap_grad, running[4] + bias_grad)
        return (updated, grad_rows)
    blank = (jnp.zeros((D, FF), jnp.float32), jnp.zeros((D, FF), jnp.float32), jnp.zeros((FF, D), jnp.float32), jnp.zeros((CONV, FF), jnp.float32), jnp.zeros((FF,), jnp.float32))
    running, grad_inputs = lax.scan(one_sequence, blank, (inputs, up_pre, gate_pre, cotangent))
    factor = float(BATCH * SEQ) ** (-0.5)
    return (grad_inputs, running[0] * factor, running[1] * factor, running[2] * factor, running[3] * factor, running[4] * factor)
```

```python
import functools
import math

import jax
import jax.numpy as jnp
from jax import lax
from jax.experimental import pallas as pl
from jax.experimental.pallas import tpu as pltpu
from jax.sharding import PartitionSpec as P

MESH = pl.DeviceIdType.MESH
F32 = jnp.float32
BF16 = jnp.bfloat16
SLOPE = math.sqrt(2.0 / math.pi)
CUBIC = 0.044715
HALO = 8
WIDE = 512
CHUNK = 256
ROWS = 128


def kernel(
    sizes,
    cot_ref,
    in_ref,
    taps_ref,
    bias_ref,
    up_hbm,
    gate_hbm,
    wdown_hbm,
    wup_hbm,
    wgate_hbm,
    gi_ref,
    fin,
    conv_out,
    cot_all,
    in_all,
    up_raw,
    gate_raw,
    wdown_f,
    wup_f,
    wgate_f,
    up_pad,
    act,
    slope_gate,
    hid,
    dconv,
    dgate,
    dup,
    down_b,
    up_b,
    gate_b,
    part,
    stage,
    conv_all,
    pair_send,
    pair_recv,
    keep,
    ring_send,
    ring_recv,
    load_sem,
    ag_send,
    ag_recv,
    part_send,
    part_recv,
    fin_send,
    fin_recv,
    conv_send,
    conv_recv,
    pair_ssem,
    pair_rsem,
    ring_ssem,
    ring_rsem,
):
    n_rep, n_fs, n_tp = sizes
    me_r, me_f, me_c = lax.axis_index("rep"), lax.axis_index("fs"), lax.axis_index("tp")
    seq, width = cot_all.shape
    ff = hid.shape[1]
    block = cot_ref.shape[0]
    taps = taps_ref.shape[0]
    per_grad = width // CHUNK
    chunks = 3 * per_grad
    me_block = me_f * n_tp + me_c

    loads = [
        pltpu.make_async_copy(src, dst, load_sem.at[at])
        for at, (src, dst) in enumerate(
            (
                (up_hbm, up_raw),
                (gate_hbm, gate_raw),
                (wdown_hbm, wdown_f),
                (wup_hbm, wup_f),
                (wgate_hbm, wgate_f),
            )
        )
    ]
    for load in loads:
        load.start()

    def other(me, step, count):
        return lax.rem(me + step, count)

    barrier = pltpu.get_barrier_semaphore()
    for axis, me, count in (("rep", me_r, n_rep), ("fs", me_f, n_fs), ("tp", me_c, n_tp)):
        for step in range(1, count):
            pl.semaphore_signal(
                barrier, inc=1, device_id={axis: other(me, step, count)}, device_id_type=MESH
            )
    pl.semaphore_wait(barrier, n_rep + n_fs + n_tp - 3)

    def remote(src, dst, send, recv, target):
        return pltpu.make_async_remote_copy(
            src_ref=src,
            dst_ref=dst,
            send_sem=send,
            recv_sem=recv,
            device_id=target,
            device_id_type=MESH,
        )

    def rows_of(index):
        return pl.ds(pl.multiple_of(index * block, block), block)

    def gather_sends(which, own_ref, whole):
        own = rows_of(me_block)
        sent = []
        for step in range(1, n_fs):
            sent.append(
                remote(
                    own_ref,
                    whole.at[own],
                    ag_send.at[which, step],
                    ag_recv.at[which, me_block],
                    {"fs": other(me_f, step, n_fs)},
                )
            )
        for step in range(1, n_tp):
            sent.append(
                remote(
                    own_ref,
                    whole.at[own],
                    ag_send.at[which, n_fs * step],
                    ag_recv.at[which, me_block],
                    {"tp": other(me_c, step, n_tp)},
                )
            )
        for copy in sent:
            copy.start()
        whole[own, :] = own_ref[...]
        return sent

    def gather_finish(which, own_ref, whole):
        passed = []
        for step in range(1, n_fs):
            source = other(me_f, n_fs - step, n_fs) * n_tp + me_c
            here = whole.at[rows_of(source)]
            remote(
                own_ref, here, ag_send.at[which, 0], ag_recv.at[which, source], {"fs": me_f}
            ).wait_recv()
            for hop in range(1, n_tp):
                copy = remote(
                    here,
                    here,
                    ag_send.at[which, n_fs * hop + step],
                    ag_recv.at[which, source],
                    {"tp": other(me_c, hop, n_tp)},
                )
                copy.start()
                passed.append(copy)
        for step in range(n_fs):
            for hop in range(1, n_tp):
                source = other(me_f, n_fs - step, n_fs) * n_tp + other(me_c, hop, n_tp)
                here = whole.at[rows_of(source)]
                remote(
                    own_ref, here, ag_send.at[which, 0], ag_recv.at[which, source], {"fs": me_f}
                ).wait_recv()
        return passed

    pending = gather_sends(0, cot_ref, cot_all)

    bias = bias_ref[...]
    weight = [taps_ref[pl.ds(k, 1), :] for k in range(taps)]
    up_pad[pl.ds(0, HALO), :] = jnp.zeros((HALO, ff), F32)
    dconv[pl.ds(seq, HALO), :] = jnp.zeros((HALO, ff), F32)
    loads[0].wait()
    loads[1].wait()

    def forward(at, _):
        rows = pl.ds(pl.multiple_of(at * ROWS, ROWS), ROWS)
        low = pl.multiple_of(at * ROWS, ROWS)
        up_pad[pl.ds(pl.multiple_of(low + HALO, HALO), ROWS), :] = up_raw[rows, :].astype(F32)
        ext = up_pad[pl.ds(low, ROWS + HALO), :]
        total = bias + jnp.zeros((ROWS, ff), F32)
        for k in range(taps):
            total = total + weight[k] * ext[HALO - k : HALO - k + ROWS]
        square = total * total
        bend = jnp.tanh(SLOPE * total * (1.0 + CUBIC * square))
        half = 0.5 * (1.0 + bend)
        active = total * half
        slope = half + 0.5 * total * (1.0 - bend * bend) * (
            SLOPE * (1.0 + 3.0 * CUBIC * square)
        )
        gate = gate_raw[rows, :].astype(F32)
        act[rows, :] = active
        hid[rows, :] = (active * gate).astype(BF16)
        slope_gate[rows, :] = slope * gate
        return 0

    lax.fori_loop(0, seq // ROWS, forward, 0)
    loads[2].wait()
    down_b[...] = wdown_f[...].astype(BF16)
    loads[3].wait()
    loads[4].wait()
    up_b[...] = wup_f[...].astype(BF16)
    gate_b[...] = wgate_f[...].astype(BF16)

    pending += gather_finish(0, cot_ref, cot_all)
    pending += gather_sends(1, in_ref, in_all)

    def owner_of(j):
        return n_rep // 2 - 1 + j % 2

    def has_away(j):
        o = owner_of(j)
        return jnp.logical_or(
            jnp.logical_and(me_r < o, me_r > 0),
            jnp.logical_and(me_r > o, me_r < n_rep - 1),
        )

    def partial_copy(j):
        o = owner_of(j)
        side = jnp.where(me_r < o, 0, 1)
        toward = jnp.clip(jnp.where(me_r < o, me_r + 1, me_r - 1), 0, n_rep - 1)
        return remote(
            stage.at[j], part.at[side, j], part_send.at[j], part_recv.at[side, j], {"rep": toward}
        )

    def wait_part(side, j):
        remote(
            stage.at[j], part.at[side, j], part_send.at[j], part_recv.at[side, j], {"rep": me_r}
        ).wait_recv()

    def final_copy(j, way):
        target = jnp.clip(me_r + (1 if way else -1), 0, n_rep - 1)
        return remote(
            fin.at[j], fin.at[j], fin_send.at[way, j], fin_recv.at[j], {"rep": target}
        )

    def is_edge(j):
        return jnp.logical_and(me_r != owner_of(j), jnp.logical_not(has_away(j)))

    def start_edge(j):
        @pl.when(is_edge(j))
        def _():
            partial_copy(j).start()

    def advance(j):
        o = owner_of(j)
        for side in (0, 1):
            inner = (me_r < o) if side == 0 else (me_r > o)

            @pl.when(jnp.logical_and(inner, has_away(j)))
            def _(side=side):
                wait_part(side, j)
                stage[j] = (stage[j].astype(F32) + part[side, j].astype(F32)).astype(BF16)
                partial_copy(j).start()

        @pl.when(me_r == o)
        def _():
            total = stage[j].astype(F32)
            if o > 0:
                wait_part(0, j)
                total = total + part[0, j].astype(F32)
            if o < n_rep - 1:
                wait_part(1, j)
                total = total + part[1, j].astype(F32)
            fin[j] = total.astype(BF16)
            if o > 0:
                final_copy(j, 0).start()
            if o < n_rep - 1:
                final_copy(j, 1).start()

    def deliver(j):
        o = owner_of(j)

        @pl.when(me_r != o)
        def _():
            final_copy(j, 0).wait_recv()

        @pl.when(jnp.logical_and(me_r < o, me_r > 0))
        def _():
            final_copy(j, 0).start()

        @pl.when(jnp.logical_and(me_r > o, me_r < n_rep - 1))
        def _():
            final_copy(j, 1).start()

    over_rows = (((0,), (0,)), ((), ()))
    over_cols = (((1,), (1,)), ((), ()))

    def weight_grad(grad, left, right):
        for piece in range(width // WIDE):
            product = lax.dot_general(
                left[...],
                right[:, pl.ds(piece * WIDE, WIDE)],
                over_rows,
                preferred_element_type=F32,
            ).astype(BF16)
            for sub in range(WIDE // CHUNK):
                j = grad * per_grad + piece * (WIDE // CHUNK) + sub
                stage[j] = product[:, sub * CHUNK : (sub + 1) * CHUNK]
                start_edge(j)

    weight_grad(0, hid, cot_all)

    def backward(at, sums):
        low = pl.multiple_of(at * ROWS, ROWS)
        rows = pl.ds(low, ROWS)
        d_hidden = (
            lax.dot_general(cot_all[rows, :], down_b[...], over_cols, preferred_element_type=F32)
            .astype(BF16)
            .astype(F32)
        )
        dgate[rows, :] = (d_hidden * act[rows, :]).astype(BF16)
        d_conv = d_hidden * slope_gate[rows, :]
        dconv[rows, :] = d_conv
        ext = up_pad[pl.ds(low, ROWS + HALO), :]
        new = [
            sums[k]
            + jnp.sum(d_conv * ext[HALO - k : HALO - k + ROWS], axis=0, keepdims=True)
            for k in range(taps)
        ]
        return (*new, sums[taps] + jnp.sum(d_conv, axis=0, keepdims=True))

    sums = lax.fori_loop(
        0, seq // ROWS, backward, tuple(jnp.zeros((1, ff), F32) for _ in range(taps + 1))
    )
    conv_all[me_r] = jnp.zeros(conv_all.shape[1:], F32)
    for k in range(taps + 1):
        conv_all[me_r, pl.ds(k, 1), :] = sums[k]

    def spread(at, _):
        low = pl.multiple_of(at * ROWS, ROWS)
        ext = dconv[pl.ds(low, ROWS + HALO), :]
        total = weight[0] * ext[0:ROWS]
        for k in range(1, taps):
            total = total + weight[k] * ext[k : k + ROWS]
        dup[pl.ds(low, ROWS), :] = total.astype(BF16)
        return 0

    lax.fori_loop(0, seq // ROWS, spread, 0)

    for step in range(1, n_rep):
        copy = remote(
            conv_all.at[me_r],
            conv_all.at[me_r],
            conv_send.at[step],
            conv_recv.at[me_r],
            {"rep": other(me_r, step, n_rep)},
        )
        copy.start()
        pending.append(copy)

    advance(0)
    pending += gather_finish(1, in_ref, in_all)
    weight_grad(1, dup, in_all)
    advance(1)
    weight_grad(2, dgate, in_all)
    advance(2)

    def input_rows(core, store):
        left_up = jnp.concatenate(
            [dup[rows_of(f * n_tp + core), :] for f in range(n_fs)], axis=0
        )
        left_gate = jnp.concatenate(
            [dgate[rows_of(f * n_tp + core), :] for f in range(n_fs)], axis=0
        )
        for piece in range(width // WIDE):
            cols = pl.ds(piece * WIDE, WIDE)
            total = lax.dot_general(
                left_up, up_b[cols, :], over_cols, preferred_element_type=F32
            ) + lax.dot_general(
                left_gate, gate_b[cols, :], over_cols, preferred_element_type=F32
            )
            store(cols, total)

    for hop in range(1, n_tp):

        def store_pair(cols, total, hop=hop):
            pair_send[hop - 1, :, cols] = total.astype(BF16)

        input_rows(other(me_c, hop, n_tp), store_pair)
        copy = remote(
            pair_send.at[hop - 1],
            pair_recv.at[hop - 1],
            pair_ssem.at[hop - 1],
            pair_rsem.at[hop - 1],
            {"tp": other(me_c, hop, n_tp)},
        )
        copy.start()
        pending.append(copy)
    deliver(0)
    advance(3)

    def store_keep(cols, total):
        keep[:, cols] = total

    input_rows(me_c, store_keep)
    for hop in range(1, n_tp):
        remote(
            pair_send.at[hop - 1],
            pair_recv.at[hop - 1],
            pair_ssem.at[hop - 1],
            pair_rsem.at[hop - 1],
            {"tp": other(me_c, hop, n_tp)},
        ).wait_recv()
    for step in range(1, n_fs):
        target = other(me_f, step, n_fs)
        rows = rows_of(target)
        total = keep[rows, :]
        for hop in range(1, n_tp):
            total = total + pair_recv[hop - 1, rows, :].astype(F32)
        ring_send[step] = total.astype(BF16)
        copy = remote(
            ring_send.at[step],
            ring_recv.at[step],
            ring_ssem.at[step],
            ring_rsem.at[step],
            {"fs": target},
        )
        copy.start()
        pending.append(copy)
    deliver(1)
    for j in range(4, chunks):
        advance(j)
        deliver(j - 2)

    own = rows_of(me_f)
    total = keep[own, :]
    for hop in range(1, n_tp):
        total = total + pair_recv[hop - 1, own, :].astype(F32)
    for step in range(1, n_fs):
        remote(
            ring_send.at[step],
            ring_recv.at[step],
            ring_ssem.at[step],
            ring_rsem.at[step],
            {"fs": me_f},
        ).wait_recv()
        total = total + ring_recv[step].astype(F32)
    gi_ref[...] = total.astype(BF16)

    for step in range(1, n_rep):
        source = other(me_r, n_rep - step, n_rep)
        remote(
            conv_all.at[source],
            conv_all.at[source],
            conv_send.at[0],
            conv_recv.at[source],
            {"rep": me_r},
        ).wait_recv()
    total = conv_all[0]
    for at in range(1, n_rep):
        total = total + conv_all[at]
    conv_out[...] = total

    for j in range(chunks - 2, chunks):
        deliver(j)

    for copy in pending:
        copy.wait_send()
    for j in range(chunks):
        o = owner_of(j)

        @pl.when(me_r != o)
        def _():
            partial_copy(j).wait_send()

        @pl.when(jnp.logical_and(me_r <= o, me_r > 0))
        def _():
            final_copy(j, 0).wait_send()

        @pl.when(jnp.logical_and(me_r >= o, me_r < n_rep - 1))
        def _():
            final_copy(j, 1).wait_send()


def on_device(
    sizes, inputs, up_pre, gate_pre, cotangent, w_up, w_gate, w_down, conv_weight, conv_bias
):
    n_rep, n_fs, n_tp = sizes
    seq, ff = up_pre.shape[1:]
    block, width = inputs.shape[1:]
    taps = conv_weight.shape[0]
    factor = float(n_rep * seq) ** (-0.5)
    chunks = 3 * width // CHUNK
    devices = n_fs * n_tp
    vmem = pl.BlockSpec(memory_space=pltpu.VMEM)
    hbm = pl.BlockSpec(memory_space=pl.ANY)
    conv_rows = -(-(taps + 1) // 8) * 8
    dma = pltpu.SemaphoreType.DMA
    grad_inputs, fin, conv = pl.pallas_call(
        functools.partial(kernel, sizes),
        out_shape=(
            jax.ShapeDtypeStruct((block, width), BF16),
            jax.ShapeDtypeStruct((chunks, ff, CHUNK), BF16),
            jax.ShapeDtypeStruct((conv_rows, ff), F32),
        ),
        in_specs=[vmem] * 4 + [hbm] * 5,
        out_specs=(vmem, vmem, vmem),
        scratch_shapes=[
            pltpu.VMEM((seq, width), BF16),
            pltpu.VMEM((seq, width), BF16),
            pltpu.VMEM((seq, ff), BF16),
            pltpu.VMEM((seq, ff), BF16),
            pltpu.VMEM((ff, width), F32),
            pltpu.VMEM((width, ff), F32),
            pltpu.VMEM((width, ff), F32),
            pltpu.VMEM((seq + HALO, ff), F32),
            pltpu.VMEM((seq, ff), F32),
            pltpu.VMEM((seq, ff), F32),
            pltpu.VMEM((seq, ff), BF16),
            pltpu.VMEM((seq + HALO, ff), F32),
            pltpu.VMEM((seq, ff), BF16),
            pltpu.VMEM((seq, ff), BF16),
            pltpu.VMEM((ff, width), BF16),
            pltpu.VMEM((width, ff), BF16),
            pltpu.VMEM((width, ff), BF16),
            pltpu.VMEM((2, chunks, ff, CHUNK), BF16),
            pltpu.VMEM((chunks, ff, CHUNK), BF16),
            pltpu.VMEM((n_rep, conv_rows, ff), F32),
            pltpu.VMEM((n_tp - 1, n_fs * block, width), BF16),
            pltpu.VMEM((n_tp - 1, n_fs * block, width), BF16),
            pltpu.VMEM((n_fs * block, width), F32),
            pltpu.VMEM((n_fs, block, width), BF16),
            pltpu.VMEM((n_fs, block, width), BF16),
            dma((5,)),
            dma((2, n_fs * n_tp)),
            dma((2, devices)),
            dma((chunks,)),
            dma((2, chunks)),
            dma((2, chunks)),
            dma((chunks,)),
            dma((n_rep,)),
            dma((n_rep,)),
            dma((n_tp,)),
            dma((n_tp,)),
            dma((n_fs,)),
            dma((n_fs,)),
        ],
        compiler_params=pltpu.CompilerParams(
            collective_id=0, has_side_effects=True, vmem_limit_bytes=62 << 20
        ),
    )(
        cotangent[0],
        inputs[0],
        conv_weight,
        conv_bias[None],
        up_pre[0],
        gate_pre[0],
        w_down,
        w_up,
        w_gate,
    )
    per_grad = width // CHUNK
    parts = fin.reshape(3, per_grad, ff, CHUNK)
    g_down = parts[0].transpose(1, 0, 2).reshape(ff, width).astype(F32) * factor
    g_up = parts[1].transpose(0, 2, 1).reshape(width, ff).astype(F32) * factor
    g_gate = parts[2].transpose(0, 2, 1).reshape(width, ff).astype(F32) * factor
    conv = conv * factor
    return grad_inputs[None], g_up, g_gate, g_down, conv[:taps], conv[taps]


def solution(mesh):
    sizes = tuple(mesh.shape[axis] for axis in ("rep", "fs", "tp"))
    return jax.shard_map(
        functools.partial(on_device, sizes),
        mesh=mesh,
        in_specs=(
            P("rep", ("fs", "tp"), None),
            P("rep", None, ("fs", "tp")),
            P("rep", None, ("fs", "tp")),
            P("rep", ("fs", "tp"), None),
            P(None, ("fs", "tp")),
            P(None, ("fs", "tp")),
            P(("fs", "tp"), None),
            P(None, ("fs", "tp")),
            P(("fs", "tp")),
        ),
        out_specs=(
            P("rep", ("fs", "tp"), None),
            P(None, ("fs", "tp")),
            P(None, ("fs", "tp")),
            P(("fs", "tp"), None),
            P(None, ("fs", "tp")),
            P(("fs", "tp")),
        ),
        check_vma=False,
    )
```

```python
import functools
import math

import jax
import jax.numpy as jnp
from jax import lax
from jax.experimental import pallas as pl
from jax.experimental.pallas import tpu as pltpu
from jax.sharding import PartitionSpec as P

MESH = pl.DeviceIdType.MESH
F32 = jnp.float32
BF16 = jnp.bfloat16
SLOPE = math.sqrt(2.0 / math.pi)
CUBIC = 0.044715
WIDE = 512
CHUNK = 256
ROWS = 16
LANES = 128


def kernel(
    sizes,
    cot_ref,
    in_ref,
    taps_ref,
    bias_ref,
    up_hbm,
    gate_hbm,
    wdown_hbm,
    wup_hbm,
    wgate_hbm,
    gi_ref,
    fin,
    taps_out,
    bias_out,
    cot_all,
    in_all,
    up_raw,
    gate_raw,
    wdown_f,
    wup_f,
    wgate_f,
    act,
    slope_gate,
    hid,
    d_hid,
    dgate,
    dup,
    down_b,
    up_b,
    gate_b,
    in_rows,
    in_cols,
    part,
    stage,
    conv_all,
    pair_send,
    pair_recv,
    keep,
    ring_send,
    ring_recv,
    load_sem,
    ag_send,
    ag_recv,
    part_send,
    part_recv,
    fin_send,
    fin_recv,
    conv_send,
    conv_recv,
    pair_ssem,
    pair_rsem,
    ring_ssem,
    ring_rsem,
):
    n_rep, n_fs, n_tp = sizes
    factor = float(n_rep * cot_all.shape[0]) ** (-0.5)
    me_r, me_f, me_c = lax.axis_index("rep"), lax.axis_index("fs"), lax.axis_index("tp")
    seq, width = cot_all.shape
    ff = hid.shape[0]
    block = cot_ref.shape[0]
    taps = taps_ref.shape[0]
    per_grad = width // CHUNK
    chunks = 3 * per_grad
    me_block = me_f * n_tp + me_c

    loads = [
        pltpu.make_async_copy(src, dst, load_sem.at[at])
        for at, (src, dst) in enumerate(
            (
                (up_hbm, up_raw),
                (gate_hbm, gate_raw),
                (wdown_hbm, wdown_f),
                (wup_hbm, wup_f),
                (wgate_hbm, wgate_f),
            )
        )
    ]
    for load in loads:
        load.start()

    def other(me, step, count):
        return lax.rem(me + step, count)

    barrier = pltpu.get_barrier_semaphore()
    for axis, me, count in (("rep", me_r, n_rep), ("fs", me_f, n_fs), ("tp", me_c, n_tp)):
        for step in range(1, count):
            pl.semaphore_signal(
                barrier, inc=1, device_id={axis: other(me, step, count)}, device_id_type=MESH
            )
    pl.semaphore_wait(barrier, n_rep + n_fs + n_tp - 3)

    def remote(src, dst, send, recv, target):
        return pltpu.make_async_remote_copy(
            src_ref=src,
            dst_ref=dst,
            send_sem=send,
            recv_sem=recv,
            device_id=target,
            device_id_type=MESH,
        )

    def rows_of(index):
        return pl.ds(pl.multiple_of(index * block, block), block)

    def gather_sends(which, own_ref, whole):
        own = rows_of(me_block)
        sent = []
        for step in range(1, n_fs):
            sent.append(
                remote(
                    own_ref,
                    whole.at[own],
                    ag_send.at[which, step],
                    ag_recv.at[which, me_block],
                    {"fs": other(me_f, step, n_fs)},
                )
            )
        for step in range(1, n_tp):
            sent.append(
                remote(
                    own_ref,
                    whole.at[own],
                    ag_send.at[which, n_fs * step],
                    ag_recv.at[which, me_block],
                    {"tp": other(me_c, step, n_tp)},
                )
            )
        for copy in sent:
            copy.start()
        whole[own, :] = own_ref[...]
        return sent

    def gather_finish(which, own_ref, whole):
        passed = []
        for step in range(1, n_fs):
            source = other(me_f, n_fs - step, n_fs) * n_tp + me_c
            here = whole.at[rows_of(source)]
            remote(
                own_ref, here, ag_send.at[which, 0], ag_recv.at[which, source], {"fs": me_f}
            ).wait_recv()
            for hop in range(1, n_tp):
                copy = remote(
                    here,
                    here,
                    ag_send.at[which, n_fs * hop + step],
                    ag_recv.at[which, source],
                    {"tp": other(me_c, hop, n_tp)},
                )
                copy.start()
                passed.append(copy)
        for step in range(n_fs):
            for hop in range(1, n_tp):
                source = other(me_f, n_fs - step, n_fs) * n_tp + other(me_c, hop, n_tp)
                here = whole.at[rows_of(source)]
                remote(
                    own_ref, here, ag_send.at[which, 0], ag_recv.at[which, source], {"fs": me_f}
                ).wait_recv()
        return passed

    pending = gather_sends(0, cot_ref, cot_all)

    in_rows[...] = jnp.zeros(in_rows.shape, F32)
    in_rows[pl.ds(0, taps), pl.ds(0, ff)] = taps_ref[...]
    in_rows[pl.ds(taps, 1), pl.ds(0, ff)] = bias_ref[...]
    in_cols[...] = in_rows[...].T
    lane = lax.broadcasted_iota(jnp.int32, (ROWS, seq), 1)

    def later(value, k):
        return value if k == 0 else jnp.where(lane >= k, pltpu.roll(value, k, 1), 0.0)

    def sooner(value, k):
        return value if k == 0 else jnp.where(lane < seq - k, pltpu.roll(value, seq - k, 1), 0.0)

    loads[0].wait()
    loads[1].wait()

    def forward(at, _):
        rows = pl.ds(pl.multiple_of(at * ROWS, ROWS), ROWS)
        up = up_raw[rows, :].astype(F32)
        total = in_cols[rows, taps : taps + 1] + jnp.zeros((ROWS, seq), F32)
        for k in range(taps):
            total = total + in_cols[rows, k : k + 1] * later(up, k)
        square = total * total
        bend = jnp.tanh(SLOPE * total * (1.0 + CUBIC * square))
        half = 0.5 * (1.0 + bend)
        active = total * half
        slope = half + 0.5 * total * (1.0 - bend * bend) * (
            SLOPE * (1.0 + 3.0 * CUBIC * square)
        )
        gate = gate_raw[rows, :].astype(F32)
        act[rows, :] = active
        hid[rows, :] = (active * gate).astype(BF16)
        slope_gate[rows, :] = slope * gate
        return 0

    lax.fori_loop(0, ff // ROWS, forward, 0)
    loads[2].wait()
    down_b[...] = wdown_f[...].astype(BF16)
    loads[3].wait()
    loads[4].wait()
    up_b[...] = wup_f[...].astype(BF16)
    gate_b[...] = wgate_f[...].astype(BF16)

    pending += gather_finish(0, cot_ref, cot_all)
    pending += gather_sends(1, in_ref, in_all)

    def owner_of(j):
        return n_rep // 2 - 1 + j % 2

    def has_away(j):
        o = owner_of(j)
        return jnp.logical_or(
            jnp.logical_and(me_r < o, me_r > 0),
            jnp.logical_and(me_r > o, me_r < n_rep - 1),
        )

    def partial_copy(j):
        o = owner_of(j)
        side = jnp.where(me_r < o, 0, 1)
        toward = jnp.clip(jnp.where(me_r < o, me_r + 1, me_r - 1), 0, n_rep - 1)
        return remote(
            stage.at[j], part.at[side, j], part_send.at[j], part_recv.at[side, j], {"rep": toward}
        )

    def wait_part(side, j):
        remote(
            stage.at[j], part.at[side, j], part_send.at[j], part_recv.at[side, j], {"rep": me_r}
        ).wait_recv()

    def spot(j):
        return j // per_grad, pl.ds(0, ff), pl.ds(j % per_grad * CHUNK, CHUNK)

    def final_copy(j, way):
        target = jnp.clip(me_r + (1 if way else -1), 0, n_rep - 1)
        return remote(
            fin.at[spot(j)], fin.at[spot(j)], fin_send.at[way, j], fin_recv.at[j], {"rep": target}
        )

    def is_edge(j):
        return jnp.logical_and(me_r != owner_of(j), jnp.logical_not(has_away(j)))

    def start_edge(j):
        @pl.when(is_edge(j))
        def _():
            partial_copy(j).start()

    def advance(j):
        o = owner_of(j)
        for side in (0, 1):
            inner = (me_r < o) if side == 0 else (me_r > o)

            @pl.when(jnp.logical_and(inner, has_away(j)))
            def _(side=side):
                wait_part(side, j)
                stage[j] = (stage[j].astype(F32) + part[side, j].astype(F32)).astype(BF16)
                partial_copy(j).start()

        @pl.when(me_r == o)
        def _():
            total = stage[j].astype(F32)
            if o > 0:
                wait_part(0, j)
                total = total + part[0, j].astype(F32)
            if o < n_rep - 1:
                wait_part(1, j)
                total = total + part[1, j].astype(F32)
            fin[spot(j)] = total.astype(BF16)
            if o > 0:
                final_copy(j, 0).start()
            if o < n_rep - 1:
                final_copy(j, 1).start()

    def deliver(j):
        o = owner_of(j)

        @pl.when(me_r != o)
        def _():
            final_copy(j, 0).wait_recv()

        @pl.when(jnp.logical_and(me_r < o, me_r > 0))
        def _():
            final_copy(j, 0).start()

        @pl.when(jnp.logical_and(me_r > o, me_r < n_rep - 1))
        def _():
            final_copy(j, 1).start()

    over_rows = (((0,), (0,)), ((), ()))
    over_cols = (((1,), (1,)), ((), ()))

    def weight_grad(grad, left, right):
        for piece in range(width // WIDE):
            product = jnp.dot(
                left[...], right[:, pl.ds(piece * WIDE, WIDE)], preferred_element_type=F32
            ).astype(BF16)
            for sub in range(WIDE // CHUNK):
                j = grad * per_grad + piece * (WIDE // CHUNK) + sub
                stage[j] = product[:, sub * CHUNK : (sub + 1) * CHUNK]
                start_edge(j)

    weight_grad(0, hid, cot_all)

    for piece in range(seq // WIDE):
        cols = pl.ds(piece * WIDE, WIDE)
        d_hid[:, cols] = lax.dot_general(
            down_b[...], cot_all[cols, :], over_cols, preferred_element_type=F32
        ).astype(BF16)
    advance(0)

    def backward(at, _):
        rows = pl.ds(pl.multiple_of(at * ROWS, ROWS), ROWS)
        d_hidden = d_hid[rows, :].astype(F32)
        dgate[rows, :] = (d_hidden * act[rows, :]).astype(BF16)
        d_conv = d_hidden * slope_gate[rows, :]
        up = up_raw[rows, :].astype(F32)
        total = jnp.zeros((ROWS, seq), F32)
        for k in range(taps):
            ahead = sooner(d_conv, k)
            total = total + in_cols[rows, k : k + 1] * ahead
            in_cols[rows, taps + 1 + k : taps + 2 + k] = jnp.sum(ahead * up, axis=1, keepdims=True)
        in_cols[rows, 2 * taps + 1 : 2 * taps + 2] = jnp.sum(d_conv, axis=1, keepdims=True)
        dup[rows, :] = total.astype(BF16)
        return 0

    lax.fori_loop(0, ff // ROWS, backward, 0)
    in_rows[...] = in_cols[...].T
    conv_all[me_r] = in_rows[pl.ds(0, 8), :]

    for step in range(1, n_rep):
        copy = remote(
            conv_all.at[me_r],
            conv_all.at[me_r],
            conv_send.at[step],
            conv_recv.at[me_r],
            {"rep": other(me_r, step, n_rep)},
        )
        copy.start()
        pending.append(copy)

    pending += gather_finish(1, in_ref, in_all)
    weight_grad(1, dup, in_all)
    advance(1)
    weight_grad(2, dgate, in_all)
    advance(2)

    def input_rows(core, store):
        left_up = jnp.concatenate(
            [dup[:, rows_of(f * n_tp + core)] for f in range(n_fs)], axis=1
        )
        left_gate = jnp.concatenate(
            [dgate[:, rows_of(f * n_tp + core)] for f in range(n_fs)], axis=1
        )
        for piece in range(width // WIDE):
            cols = pl.ds(piece * WIDE, WIDE)
            total = lax.dot_general(
                left_up, up_b[:, cols], over_rows, preferred_element_type=F32
            ) + lax.dot_general(
                left_gate, gate_b[:, cols], over_rows, preferred_element_type=F32
            )
            store(cols, total)

    for hop in range(1, n_tp):

        def store_pair(cols, total, hop=hop):
            pair_send[hop - 1, :, cols] = total.astype(BF16)

        input_rows(other(me_c, hop, n_tp), store_pair)
        copy = remote(
            pair_send.at[hop - 1],
            pair_recv.at[hop - 1],
            pair_ssem.at[hop - 1],
            pair_rsem.at[hop - 1],
            {"tp": other(me_c, hop, n_tp)},
        )
        copy.start()
        pending.append(copy)
    deliver(0)
    advance(3)

    def store_keep(cols, total):
        keep[:, cols] = total

    input_rows(me_c, store_keep)
    for hop in range(1, n_tp):
        remote(
            pair_send.at[hop - 1],
            pair_recv.at[hop - 1],
            pair_ssem.at[hop - 1],
            pair_rsem.at[hop - 1],
            {"tp": other(me_c, hop, n_tp)},
        ).wait_recv()
    for step in range(1, n_fs):
        target = other(me_f, step, n_fs)
        rows = rows_of(target)
        total = keep[rows, :]
        for hop in range(1, n_tp):
            total = total + pair_recv[hop - 1, rows, :].astype(F32)
        ring_send[step] = total.astype(BF16)
        copy = remote(
            ring_send.at[step],
            ring_recv.at[step],
            ring_ssem.at[step],
            ring_rsem.at[step],
            {"fs": target},
        )
        copy.start()
        pending.append(copy)
    deliver(1)
    for j in range(4, chunks):
        advance(j)
        deliver(j - 2)

    own = rows_of(me_f)
    total = keep[own, :]
    for hop in range(1, n_tp):
        total = total + pair_recv[hop - 1, own, :].astype(F32)
    for step in range(1, n_fs):
        remote(
            ring_send.at[step],
            ring_recv.at[step],
            ring_ssem.at[step],
            ring_rsem.at[step],
            {"fs": me_f},
        ).wait_recv()
        total = total + ring_recv[step].astype(F32)
    gi_ref[...] = total.astype(BF16)

    for step in range(1, n_rep):
        source = other(me_r, n_rep - step, n_rep)
        remote(
            conv_all.at[source],
            conv_all.at[source],
            conv_send.at[0],
            conv_recv.at[source],
            {"rep": me_r},
        ).wait_recv()
    total = conv_all[0]
    for at in range(1, n_rep):
        total = total + conv_all[at]
    taps_out[...] = total[taps + 1 : 2 * taps + 1, :ff] * factor
    bias_out[...] = total[2 * taps + 1 : 2 * taps + 2, :ff] * factor

    for j in range(chunks - 2, chunks):
        deliver(j)

    for copy in pending:
        copy.wait_send()
    for j in range(chunks):
        o = owner_of(j)

        @pl.when(me_r != o)
        def _():
            partial_copy(j).wait_send()

        @pl.when(jnp.logical_and(me_r <= o, me_r > 0))
        def _():
            final_copy(j, 0).wait_send()

        @pl.when(jnp.logical_and(me_r >= o, me_r < n_rep - 1))
        def _():
            final_copy(j, 1).wait_send()


def on_device(
    sizes, inputs, up_pre, gate_pre, cotangent, w_up, w_gate, w_down, conv_weight, conv_bias
):
    n_rep, n_fs, n_tp = sizes
    seq, ff = up_pre.shape[1:]
    block, width = inputs.shape[1:]
    taps = conv_weight.shape[0]
    factor = float(n_rep * seq) ** (-0.5)
    chunks = 3 * width // CHUNK
    devices = n_fs * n_tp
    vmem = pl.BlockSpec(memory_space=pltpu.VMEM)
    hbm = pl.BlockSpec(memory_space=pl.ANY)
    dma = pltpu.SemaphoreType.DMA
    padded = -(-ff // LANES) * LANES
    grad_inputs, fin, g_taps, g_bias = pl.pallas_call(
        functools.partial(kernel, sizes),
        out_shape=(
            jax.ShapeDtypeStruct((block, width), BF16),
            jax.ShapeDtypeStruct((3, ff, width), BF16),
            jax.ShapeDtypeStruct((taps, ff), F32),
            jax.ShapeDtypeStruct((1, ff), F32),
        ),
        in_specs=[vmem] * 4 + [hbm] * 5,
        out_specs=(vmem,) * 4,
        scratch_shapes=[
            pltpu.VMEM((seq, width), BF16),
            pltpu.VMEM((seq, width), BF16),
            pltpu.VMEM((ff, seq), BF16),
            pltpu.VMEM((ff, seq), BF16),
            pltpu.VMEM((ff, width), F32),
            pltpu.VMEM((ff, width), F32),
            pltpu.VMEM((ff, width), F32),
            pltpu.VMEM((ff, seq), F32),
            pltpu.VMEM((ff, seq), F32),
            pltpu.VMEM((ff, seq), BF16),
            pltpu.VMEM((ff, seq), BF16),
            pltpu.VMEM((ff, seq), BF16),
            pltpu.VMEM((ff, seq), BF16),
            pltpu.VMEM((ff, width), BF16),
            pltpu.VMEM((ff, width), BF16),
            pltpu.VMEM((ff, width), BF16),
            pltpu.VMEM((LANES, padded), F32),
            pltpu.VMEM((padded, LANES), F32),
            pltpu.VMEM((2, chunks, ff, CHUNK), BF16),
            pltpu.VMEM((chunks, ff, CHUNK), BF16),
            pltpu.VMEM((n_rep, 8, padded), F32),
            pltpu.VMEM((n_tp - 1, n_fs * block, width), BF16),
            pltpu.VMEM((n_tp - 1, n_fs * block, width), BF16),
            pltpu.VMEM((n_fs * block, width), F32),
            pltpu.VMEM((n_fs, block, width), BF16),
            pltpu.VMEM((n_fs, block, width), BF16),
            dma((5,)),
            dma((2, n_fs * n_tp)),
            dma((2, devices)),
            dma((chunks,)),
            dma((2, chunks)),
            dma((2, chunks)),
            dma((chunks,)),
            dma((n_rep,)),
            dma((n_rep,)),
            dma((n_tp,)),
            dma((n_tp,)),
            dma((n_fs,)),
            dma((n_fs,)),
        ],
        compiler_params=pltpu.CompilerParams(
            collective_id=0, has_side_effects=True, vmem_limit_bytes=62 << 20
        ),
    )(
        cotangent[0],
        inputs[0],
        conv_weight,
        conv_bias[None],
        up_pre[0].T,
        gate_pre[0].T,
        w_down,
        w_up.T,
        w_gate.T,
    )
    g_down = fin[0].astype(F32) * factor
    g_up = fin[1].T.astype(F32) * factor
    g_gate = fin[2].T.astype(F32) * factor
    return grad_inputs[None], g_up, g_gate, g_down, g_taps, g_bias[0]


def solution(mesh):
    sizes = tuple(mesh.shape[axis] for axis in ("rep", "fs", "tp"))
    return jax.shard_map(
        functools.partial(on_device, sizes),
        mesh=mesh,
        in_specs=(
            P("rep", ("fs", "tp"), None),
            P("rep", None, ("fs", "tp")),
            P("rep", None, ("fs", "tp")),
            P("rep", ("fs", "tp"), None),
            P(None, ("fs", "tp")),
            P(None, ("fs", "tp")),
            P(("fs", "tp"), None),
            P(None, ("fs", "tp")),
            P(("fs", "tp")),
        ),
        out_specs=(
            P("rep", ("fs", "tp"), None),
            P(None, ("fs", "tp")),
            P(None, ("fs", "tp")),
            P(("fs", "tp"), None),
            P(None, ("fs", "tp")),
            P(("fs", "tp")),
        ),
        check_vma=False,
    )
```

```python
import functools
import math

import jax
import jax.numpy as jnp
from jax import lax
from jax.experimental import pallas as pl
from jax.experimental.pallas import tpu as pltpu
from jax.sharding import PartitionSpec as P

MESH = pl.DeviceIdType.MESH
F32 = jnp.float32
BF16 = jnp.bfloat16
SLOPE = math.sqrt(2.0 / math.pi)
CUBIC = 0.044715
WIDE = 512
CHUNK = 256
FLIGHT = 2
OWN_LAG = 2
LAG = 5
ROWS = 16
LANES = 128


def kernel(
    sizes,
    cot_ref,
    in_ref,
    taps_ref,
    bias_ref,
    up_hbm,
    gate_hbm,
    wdown_hbm,
    wup_hbm,
    wgate_hbm,
    gi_ref,
    fin,
    taps_out,
    bias_out,
    cot_all,
    in_all,
    up_raw,
    gate_raw,
    wdown_f,
    wup_f,
    wgate_f,
    act,
    slope_gate,
    hid,
    d_hid,
    dgate,
    dup,
    down_b,
    up_b,
    gate_b,
    in_rows,
    in_cols,
    part,
    stage,
    land,
    conv_all,
    pair_send,
    pair_recv,
    keep,
    ring_send,
    ring_recv,
    load_sem,
    ag_send,
    ag_recv,
    part_send,
    part_recv,
    fin_send,
    fin_recv,
    conv_send,
    conv_recv,
    pair_ssem,
    pair_rsem,
    ring_ssem,
    ring_rsem,
):
    n_rep, n_fs, n_tp = sizes
    factor = float(n_rep * cot_all.shape[0]) ** (-0.5)
    me_r, me_f, me_c = lax.axis_index("rep"), lax.axis_index("fs"), lax.axis_index("tp")
    seq, width = cot_all.shape
    ff = hid.shape[0]
    block = cot_ref.shape[0]
    taps = taps_ref.shape[0]
    per_grad = width // CHUNK
    chunks = 3 * per_grad
    me_block = me_f * n_tp + me_c

    loads = [
        pltpu.make_async_copy(src, dst, load_sem.at[at])
        for at, (src, dst) in enumerate(
            (
                (up_hbm, up_raw),
                (gate_hbm, gate_raw),
                (wdown_hbm, wdown_f),
                (wup_hbm, wup_f),
                (wgate_hbm, wgate_f),
            )
        )
    ]
    for load in loads:
        load.start()

    def other(me, step, count):
        return lax.rem(me + step, count)

    barrier = pltpu.get_barrier_semaphore()
    for axis, me, count in (("rep", me_r, n_rep), ("fs", me_f, n_fs), ("tp", me_c, n_tp)):
        for step in range(1, count):
            pl.semaphore_signal(
                barrier, inc=1, device_id={axis: other(me, step, count)}, device_id_type=MESH
            )
    pl.semaphore_wait(barrier, n_rep + n_fs + n_tp - 3)

    def remote(src, dst, send, recv, target):
        return pltpu.make_async_remote_copy(
            src_ref=src,
            dst_ref=dst,
            send_sem=send,
            recv_sem=recv,
            device_id=target,
            device_id_type=MESH,
        )

    def rows_of(index):
        return pl.ds(pl.multiple_of(index * block, block), block)

    def gather_sends(which, own_ref, whole):
        own = rows_of(me_block)
        sent = []
        for step in range(1, n_fs):
            sent.append(
                remote(
                    own_ref,
                    whole.at[own],
                    ag_send.at[which, step],
                    ag_recv.at[which, me_block],
                    {"fs": other(me_f, step, n_fs)},
                )
            )
        for step in range(1, n_tp):
            sent.append(
                remote(
                    own_ref,
                    whole.at[own],
                    ag_send.at[which, n_fs * step],
                    ag_recv.at[which, me_block],
                    {"tp": other(me_c, step, n_tp)},
                )
            )
        for copy in sent:
            copy.start()
        whole[own, :] = own_ref[...]
        return sent

    def gather_finish(which, own_ref, whole):
        passed = []
        for step in range(1, n_fs):
            source = other(me_f, n_fs - step, n_fs) * n_tp + me_c
            here = whole.at[rows_of(source)]
            remote(
                own_ref, here, ag_send.at[which, 0], ag_recv.at[which, source], {"fs": me_f}
            ).wait_recv()
            for hop in range(1, n_tp):
                copy = remote(
                    here,
                    here,
                    ag_send.at[which, n_fs * hop + step],
                    ag_recv.at[which, source],
                    {"tp": other(me_c, hop, n_tp)},
                )
                copy.start()
                passed.append(copy)
        for step in range(n_fs):
            for hop in range(1, n_tp):
                source = other(me_f, n_fs - step, n_fs) * n_tp + other(me_c, hop, n_tp)
                here = whole.at[rows_of(source)]
                remote(
                    own_ref, here, ag_send.at[which, 0], ag_recv.at[which, source], {"fs": me_f}
                ).wait_recv()
        return passed

    pending = gather_sends(0, cot_ref, cot_all)

    in_rows[...] = jnp.zeros(in_rows.shape, F32)
    in_rows[pl.ds(0, taps), pl.ds(0, ff)] = taps_ref[...]
    in_rows[pl.ds(taps, 1), pl.ds(0, ff)] = bias_ref[...]
    in_cols[...] = in_rows[...].T
    lane = lax.broadcasted_iota(jnp.int32, (ROWS, seq), 1)

    def later(value, k):
        return value if k == 0 else jnp.where(lane >= k, pltpu.roll(value, k, 1), 0.0)

    def sooner(value, k):
        return value if k == 0 else jnp.where(lane < seq - k, pltpu.roll(value, seq - k, 1), 0.0)

    loads[0].wait()
    loads[1].wait()

    def forward(at, _):
        rows = pl.ds(pl.multiple_of(at * ROWS, ROWS), ROWS)
        up = up_raw[rows, :].astype(F32)
        total = in_cols[rows, taps : taps + 1] + jnp.zeros((ROWS, seq), F32)
        for k in range(taps):
            total = total + in_cols[rows, k : k + 1] * later(up, k)
        square = total * total
        bend = jnp.tanh(SLOPE * total * (1.0 + CUBIC * square))
        half = 0.5 * (1.0 + bend)
        active = total * half
        slope = half + 0.5 * total * (1.0 - bend * bend) * (
            SLOPE * (1.0 + 3.0 * CUBIC * square)
        )
        gate = gate_raw[rows, :].astype(F32)
        act[rows, :] = active
        hid[rows, :] = (active * gate).astype(BF16)
        slope_gate[rows, :] = slope * gate
        return 0

    lax.fori_loop(0, ff // ROWS, forward, 0)
    loads[2].wait()
    down_b[...] = wdown_f[...].astype(BF16)
    loads[3].wait()
    loads[4].wait()
    up_b[...] = wup_f[...].astype(BF16)
    gate_b[...] = wgate_f[...].astype(BF16)

    pending += gather_finish(0, cot_ref, cot_all)
    pending += gather_sends(1, in_ref, in_all)

    def owner_of(j):
        return n_rep // 2 - 1 + j % 2

    def has_away(j):
        o = owner_of(j)
        return jnp.logical_or(
            jnp.logical_and(me_r < o, me_r > 0),
            jnp.logical_and(me_r > o, me_r < n_rep - 1),
        )

    def partial_copy(j):
        o = owner_of(j)
        side = jnp.where(me_r < o, 0, 1)
        toward = jnp.clip(jnp.where(me_r < o, me_r + 1, me_r - 1), 0, n_rep - 1)
        return remote(
            stage.at[j], part.at[side, j], part_send.at[j], part_recv.at[side, j], {"rep": toward}
        )

    def wait_part(side, j):
        remote(
            stage.at[j], part.at[side, j], part_send.at[j], part_recv.at[side, j], {"rep": me_r}
        ).wait_recv()

    def spot(j):
        return j // per_grad, pl.ds(0, ff), pl.ds(j % per_grad * CHUNK, CHUNK)

    def final_copy(j, way):
        target = jnp.clip(me_r + (1 if way else -1), 0, n_rep - 1)
        return remote(
            land.at[j], land.at[j], fin_send.at[way, j], fin_recv.at[j], {"rep": target}
        )

    def is_edge(j):
        return jnp.logical_and(me_r != owner_of(j), jnp.logical_not(has_away(j)))

    def start_edge(j):
        @pl.when(is_edge(j))
        def _():
            partial_copy(j).start()

    def pass_on(j):
        o = owner_of(j)
        if j + FLIGHT < chunks:

            @pl.when(is_edge(j))
            def _():
                partial_copy(j).wait_send()
                partial_copy(j + FLIGHT).start()

        for side in (0, 1):
            inner = (me_r < o) if side == 0 else (me_r > o)

            @pl.when(jnp.logical_and(inner, has_away(j)))
            def _(side=side):
                wait_part(side, j)
                stage[j] = (stage[j].astype(F32) + part[side, j].astype(F32)).astype(BF16)
                partial_copy(j).start()

    def own_sum(j):
        o = owner_of(j)

        @pl.when(me_r == o)
        def _():
            total = stage[j].astype(F32)
            if o > 0:
                wait_part(0, j)
                total = total + part[0, j].astype(F32)
            if o < n_rep - 1:
                wait_part(1, j)
                total = total + part[1, j].astype(F32)
            land[j] = total.astype(BF16)
            if o > 0:
                final_copy(j, 0).start()
            if o < n_rep - 1:
                final_copy(j, 1).start()

    def deliver(j):
        o = owner_of(j)

        @pl.when(me_r != o)
        def _():
            final_copy(j, 0).wait_recv()

        @pl.when(jnp.logical_and(me_r < o, me_r > 0))
        def _():
            final_copy(j, 0).start()

        @pl.when(jnp.logical_and(me_r > o, me_r < n_rep - 1))
        def _():
            final_copy(j, 1).start()

    def settle(j):
        deliver(j)
        fin[spot(j)] = land[j]

    def advance(k):
        if k < chunks:
            pass_on(k)
        if 0 <= k - OWN_LAG < chunks:
            own_sum(k - OWN_LAG)
        if 0 <= k - LAG < chunks:
            settle(k - LAG)

    over_rows = (((0,), (0,)), ((), ()))
    over_cols = (((1,), (1,)), ((), ()))

    def weight_grad(grad, left, right):
        for piece in range(width // WIDE):
            product = jnp.dot(
                left[...], right[:, pl.ds(piece * WIDE, WIDE)], preferred_element_type=F32
            ).astype(BF16)
            for sub in range(WIDE // CHUNK):
                j = grad * per_grad + piece * (WIDE // CHUNK) + sub
                stage[j] = product[:, sub * CHUNK : (sub + 1) * CHUNK]
                if j < FLIGHT:
                    start_edge(j)

    weight_grad(0, hid, cot_all)

    for piece in range(seq // WIDE):
        cols = pl.ds(piece * WIDE, WIDE)
        d_hid[:, cols] = lax.dot_general(
            down_b[...], cot_all[cols, :], over_cols, preferred_element_type=F32
        ).astype(BF16)
    advance(0)

    def backward(at, _):
        rows = pl.ds(pl.multiple_of(at * ROWS, ROWS), ROWS)
        d_hidden = d_hid[rows, :].astype(F32)
        dgate[rows, :] = (d_hidden * act[rows, :]).astype(BF16)
        d_conv = d_hidden * slope_gate[rows, :]
        up = up_raw[rows, :].astype(F32)
        total = jnp.zeros((ROWS, seq), F32)
        for k in range(taps):
            ahead = sooner(d_conv, k)
            total = total + in_cols[rows, k : k + 1] * ahead
            in_cols[rows, taps + 1 + k : taps + 2 + k] = jnp.sum(ahead * up, axis=1, keepdims=True)
        in_cols[rows, 2 * taps + 1 : 2 * taps + 2] = jnp.sum(d_conv, axis=1, keepdims=True)
        dup[rows, :] = total.astype(BF16)
        return 0

    lax.fori_loop(0, ff // ROWS, backward, 0)
    in_rows[...] = in_cols[...].T
    conv_all[me_r] = in_rows[pl.ds(0, 8), :]

    for step in range(1, n_rep):
        copy = remote(
            conv_all.at[me_r],
            conv_all.at[me_r],
            conv_send.at[step],
            conv_recv.at[me_r],
            {"rep": other(me_r, step, n_rep)},
        )
        copy.start()
        pending.append(copy)

    pending += gather_finish(1, in_ref, in_all)
    weight_grad(1, dup, in_all)
    advance(1)
    weight_grad(2, dgate, in_all)
    advance(2)

    def input_rows(core, store):
        left_up = jnp.concatenate(
            [dup[:, rows_of(f * n_tp + core)] for f in range(n_fs)], axis=1
        )
        left_gate = jnp.concatenate(
            [dgate[:, rows_of(f * n_tp + core)] for f in range(n_fs)], axis=1
        )
        for piece in range(width // WIDE):
            cols = pl.ds(piece * WIDE, WIDE)
            total = lax.dot_general(
                left_up, up_b[:, cols], over_rows, preferred_element_type=F32
            ) + lax.dot_general(
                left_gate, gate_b[:, cols], over_rows, preferred_element_type=F32
            )
            store(cols, total)

    for hop in range(1, n_tp):

        def store_pair(cols, total, hop=hop):
            pair_send[hop - 1, :, cols] = total.astype(BF16)

        input_rows(other(me_c, hop, n_tp), store_pair)
        copy = remote(
            pair_send.at[hop - 1],
            pair_recv.at[hop - 1],
            pair_ssem.at[hop - 1],
            pair_rsem.at[hop - 1],
            {"tp": other(me_c, hop, n_tp)},
        )
        copy.start()
        pending.append(copy)
    advance(3)

    def store_keep(cols, total):
        keep[:, cols] = total

    input_rows(me_c, store_keep)
    for hop in range(1, n_tp):
        remote(
            pair_send.at[hop - 1],
            pair_recv.at[hop - 1],
            pair_ssem.at[hop - 1],
            pair_rsem.at[hop - 1],
            {"tp": other(me_c, hop, n_tp)},
        ).wait_recv()
    for step in range(1, n_fs):
        target = other(me_f, step, n_fs)
        rows = rows_of(target)
        total = keep[rows, :]
        for hop in range(1, n_tp):
            total = total + pair_recv[hop - 1, rows, :].astype(F32)
        ring_send[step] = total.astype(BF16)
        copy = remote(
            ring_send.at[step],
            ring_recv.at[step],
            ring_ssem.at[step],
            ring_rsem.at[step],
            {"fs": target},
        )
        copy.start()
        pending.append(copy)
    for j in range(4, chunks):
        advance(j)

    own = rows_of(me_f)
    total = keep[own, :]
    for hop in range(1, n_tp):
        total = total + pair_recv[hop - 1, own, :].astype(F32)
    for step in range(1, n_fs):
        remote(
            ring_send.at[step],
            ring_recv.at[step],
            ring_ssem.at[step],
            ring_rsem.at[step],
            {"fs": me_f},
        ).wait_recv()
        total = total + ring_recv[step].astype(F32)
    gi_ref[...] = total.astype(BF16)

    for step in range(1, n_rep):
        source = other(me_r, n_rep - step, n_rep)
        remote(
            conv_all.at[source],
            conv_all.at[source],
            conv_send.at[0],
            conv_recv.at[source],
            {"rep": me_r},
        ).wait_recv()
    total = conv_all[0]
    for at in range(1, n_rep):
        total = total + conv_all[at]
    taps_out[...] = total[taps + 1 : 2 * taps + 1, :ff] * factor
    bias_out[...] = total[2 * taps + 1 : 2 * taps + 2, :ff] * factor

    for j in range(chunks, chunks + LAG):
        advance(j)

    for copy in pending:
        copy.wait_send()
    for j in range(chunks):
        o = owner_of(j)

        unsent = me_r != o
        if j + FLIGHT < chunks:
            unsent = jnp.logical_and(unsent, has_away(j))

        @pl.when(unsent)
        def _():
            partial_copy(j).wait_send()

        @pl.when(jnp.logical_and(me_r <= o, me_r > 0))
        def _():
            final_copy(j, 0).wait_send()

        @pl.when(jnp.logical_and(me_r >= o, me_r < n_rep - 1))
        def _():
            final_copy(j, 1).wait_send()


def on_device(
    sizes, inputs, up_pre, gate_pre, cotangent, w_up, w_gate, w_down, conv_weight, conv_bias
):
    n_rep, n_fs, n_tp = sizes
    seq, ff = up_pre.shape[1:]
    block, width = inputs.shape[1:]
    taps = conv_weight.shape[0]
    factor = float(n_rep * seq) ** (-0.5)
    chunks = 3 * width // CHUNK
    devices = n_fs * n_tp
    vmem = pl.BlockSpec(memory_space=pltpu.VMEM)
    hbm = pl.BlockSpec(memory_space=pl.ANY)
    dma = pltpu.SemaphoreType.DMA
    padded = -(-ff // LANES) * LANES
    grad_inputs, fin, g_taps, g_bias = pl.pallas_call(
        functools.partial(kernel, sizes),
        out_shape=(
            jax.ShapeDtypeStruct((block, width), BF16),
            jax.ShapeDtypeStruct((3, ff, width), BF16),
            jax.ShapeDtypeStruct((taps, ff), F32),
            jax.ShapeDtypeStruct((1, ff), F32),
        ),
        in_specs=[vmem] * 4 + [hbm] * 5,
        out_specs=(vmem,) * 4,
        scratch_shapes=[
            pltpu.VMEM((seq, width), BF16),
            pltpu.VMEM((seq, width), BF16),
            pltpu.VMEM((ff, seq), BF16),
            pltpu.VMEM((ff, seq), BF16),
            pltpu.VMEM((ff, width), F32),
            pltpu.VMEM((ff, width), F32),
            pltpu.VMEM((ff, width), F32),
            pltpu.VMEM((ff, seq), F32),
            pltpu.VMEM((ff, seq), F32),
            pltpu.VMEM((ff, seq), BF16),
            pltpu.VMEM((ff, seq), BF16),
            pltpu.VMEM((ff, seq), BF16),
            pltpu.VMEM((ff, seq), BF16),
            pltpu.VMEM((ff, width), BF16),
            pltpu.VMEM((ff, width), BF16),
            pltpu.VMEM((ff, width), BF16),
            pltpu.VMEM((LANES, padded), F32),
            pltpu.VMEM((padded, LANES), F32),
            pltpu.VMEM((2, chunks, ff, CHUNK), BF16),
            pltpu.VMEM((chunks, ff, CHUNK), BF16),
            pltpu.VMEM((chunks, ff, CHUNK), BF16),
            pltpu.VMEM((n_rep, 8, padded), F32),
            pltpu.VMEM((n_tp - 1, n_fs * block, width), BF16),
            pltpu.VMEM((n_tp - 1, n_fs * block, width), BF16),
            pltpu.VMEM((n_fs * block, width), F32),
            pltpu.VMEM((n_fs, block, width), BF16),
            pltpu.VMEM((n_fs, block, width), BF16),
            dma((5,)),
            dma((2, n_fs * n_tp)),
            dma((2, devices)),
            dma((chunks,)),
            dma((2, chunks)),
            dma((2, chunks)),
            dma((chunks,)),
            dma((n_rep,)),
            dma((n_rep,)),
            dma((n_tp,)),
            dma((n_tp,)),
            dma((n_fs,)),
            dma((n_fs,)),
        ],
        compiler_params=pltpu.CompilerParams(
            collective_id=0, has_side_effects=True, vmem_limit_bytes=62 << 20
        ),
    )(
        cotangent[0],
        inputs[0],
        conv_weight,
        conv_bias[None],
        up_pre[0].T,
        gate_pre[0].T,
        w_down,
        w_up.T,
        w_gate.T,
    )
    g_down = fin[0].astype(F32) * factor
    g_up = fin[1].T.astype(F32) * factor
    g_gate = fin[2].T.astype(F32) * factor
    return grad_inputs[None], g_up, g_gate, g_down, g_taps, g_bias[0]


def solution(mesh):
    sizes = tuple(mesh.shape[axis] for axis in ("rep", "fs", "tp"))
    return jax.shard_map(
        functools.partial(on_device, sizes),
        mesh=mesh,
        in_specs=(
            P("rep", ("fs", "tp"), None),
            P("rep", None, ("fs", "tp")),
            P("rep", None, ("fs", "tp")),
            P("rep", ("fs", "tp"), None),
            P(None, ("fs", "tp")),
            P(None, ("fs", "tp")),
            P(("fs", "tp"), None),
            P(None, ("fs", "tp")),
            P(("fs", "tp")),
        ),
        out_specs=(
            P("rep", ("fs", "tp"), None),
            P(None, ("fs", "tp")),
            P(None, ("fs", "tp")),
            P(("fs", "tp"), None),
            P(None, ("fs", "tp")),
            P(("fs", "tp")),
        ),
        check_vma=False,
    )
```

```python
import functools
import math

import jax
import jax.numpy as jnp
from jax import lax
from jax.experimental import pallas as pl
from jax.experimental.pallas import tpu as pltpu
from jax.sharding import PartitionSpec as P

MESH = pl.DeviceIdType.MESH
F32 = jnp.float32
BF16 = jnp.bfloat16
SLOPE = math.sqrt(2.0 / math.pi)
CUBIC = 0.044715
WIDE = 512
CHUNK = 256
FLIGHT = 4
OWN_LAG = 2
LAG = 5
ROWS = 16
LANES = 128


def kernel(
    sizes,
    cot_ref,
    in_ref,
    taps_ref,
    bias_ref,
    up_hbm,
    gate_hbm,
    wdown_hbm,
    wup_hbm,
    wgate_hbm,
    gi_ref,
    fin,
    taps_out,
    bias_out,
    cot_all,
    in_all,
    up_raw,
    gate_raw,
    wdown_f,
    wup_f,
    wgate_f,
    act,
    slope_gate,
    hid,
    d_hid,
    dgate,
    dup,
    down_b,
    up_b,
    gate_b,
    in_rows,
    in_cols,
    part,
    stage,
    land,
    conv_all,
    pair_send,
    pair_recv,
    keep,
    ring_send,
    ring_recv,
    load_sem,
    ag_send,
    ag_recv,
    part_send,
    part_recv,
    fin_send,
    fin_recv,
    conv_send,
    conv_recv,
    pair_ssem,
    pair_rsem,
    ring_ssem,
    ring_rsem,
):
    n_rep, n_fs, n_tp = sizes
    factor = float(n_rep * cot_all.shape[0]) ** (-0.5)
    me_r, me_f, me_c = lax.axis_index("rep"), lax.axis_index("fs"), lax.axis_index("tp")
    seq, width = cot_all.shape
    ff = hid.shape[0]
    block = cot_ref.shape[0]
    taps = taps_ref.shape[0]
    per_grad = width // CHUNK
    chunks = 3 * per_grad
    me_block = me_f * n_tp + me_c

    loads = [
        pltpu.make_async_copy(src, dst, load_sem.at[at])
        for at, (src, dst) in enumerate(
            (
                (up_hbm, up_raw),
                (gate_hbm, gate_raw),
                (wdown_hbm, wdown_f),
                (wup_hbm, wup_f),
                (wgate_hbm, wgate_f),
            )
        )
    ]
    for load in loads:
        load.start()

    def other(me, step, count):
        return lax.rem(me + step, count)

    barrier = pltpu.get_barrier_semaphore()
    for axis, me, count in (("rep", me_r, n_rep), ("fs", me_f, n_fs), ("tp", me_c, n_tp)):
        for step in range(1, count):
            pl.semaphore_signal(
                barrier, inc=1, device_id={axis: other(me, step, count)}, device_id_type=MESH
            )
    pl.semaphore_wait(barrier, n_rep + n_fs + n_tp - 3)

    def remote(src, dst, send, recv, target):
        return pltpu.make_async_remote_copy(
            src_ref=src,
            dst_ref=dst,
            send_sem=send,
            recv_sem=recv,
            device_id=target,
            device_id_type=MESH,
        )

    def rows_of(index):
        return pl.ds(pl.multiple_of(index * block, block), block)

    def gather_sends(which, own_ref, whole):
        own = rows_of(me_block)
        sent = []
        for step in range(1, n_fs):
            sent.append(
                remote(
                    own_ref,
                    whole.at[own],
                    ag_send.at[which, step],
                    ag_recv.at[which, me_block],
                    {"fs": other(me_f, step, n_fs)},
                )
            )
        for step in range(1, n_tp):
            sent.append(
                remote(
                    own_ref,
                    whole.at[own],
                    ag_send.at[which, n_fs * step],
                    ag_recv.at[which, me_block],
                    {"tp": other(me_c, step, n_tp)},
                )
            )
        for copy in sent:
            copy.start()
        whole[own, :] = own_ref[...]
        return sent

    def gather_finish(which, own_ref, whole):
        passed = []
        for step in range(1, n_fs):
            source = other(me_f, n_fs - step, n_fs) * n_tp + me_c
            here = whole.at[rows_of(source)]
            remote(
                own_ref, here, ag_send.at[which, 0], ag_recv.at[which, source], {"fs": me_f}
            ).wait_recv()
            for hop in range(1, n_tp):
                copy = remote(
                    here,
                    here,
                    ag_send.at[which, n_fs * hop + step],
                    ag_recv.at[which, source],
                    {"tp": other(me_c, hop, n_tp)},
                )
                copy.start()
                passed.append(copy)
        for step in range(n_fs):
            for hop in range(1, n_tp):
                source = other(me_f, n_fs - step, n_fs) * n_tp + other(me_c, hop, n_tp)
                here = whole.at[rows_of(source)]
                remote(
                    own_ref, here, ag_send.at[which, 0], ag_recv.at[which, source], {"fs": me_f}
                ).wait_recv()
        return passed

    pending = gather_sends(0, cot_ref, cot_all)

    in_rows[...] = jnp.zeros(in_rows.shape, F32)
    in_rows[pl.ds(0, taps), pl.ds(0, ff)] = taps_ref[...]
    in_rows[pl.ds(taps, 1), pl.ds(0, ff)] = bias_ref[...]
    in_cols[...] = in_rows[...].T
    lane = lax.broadcasted_iota(jnp.int32, (ROWS, seq), 1)

    def later(value, k):
        return value if k == 0 else jnp.where(lane >= k, pltpu.roll(value, k, 1), 0.0)

    def sooner(value, k):
        return value if k == 0 else jnp.where(lane < seq - k, pltpu.roll(value, seq - k, 1), 0.0)

    loads[0].wait()
    loads[1].wait()

    def forward(at, _):
        rows = pl.ds(pl.multiple_of(at * ROWS, ROWS), ROWS)
        up = up_raw[rows, :].astype(F32)
        total = in_cols[rows, taps : taps + 1] + jnp.zeros((ROWS, seq), F32)
        for k in range(taps):
            total = total + in_cols[rows, k : k + 1] * later(up, k)
        square = total * total
        bend = jnp.tanh(SLOPE * total * (1.0 + CUBIC * square))
        half = 0.5 * (1.0 + bend)
        active = total * half
        slope = half + 0.5 * total * (1.0 - bend * bend) * (
            SLOPE * (1.0 + 3.0 * CUBIC * square)
        )
        gate = gate_raw[rows, :].astype(F32)
        act[rows, :] = active
        hid[rows, :] = (active * gate).astype(BF16)
        slope_gate[rows, :] = slope * gate
        return 0

    lax.fori_loop(0, ff // ROWS, forward, 0)
    loads[2].wait()
    down_b[...] = wdown_f[...].astype(BF16)
    loads[3].wait()
    loads[4].wait()
    up_b[...] = wup_f[...].astype(BF16)
    gate_b[...] = wgate_f[...].astype(BF16)

    pending += gather_finish(0, cot_ref, cot_all)
    pending += gather_sends(1, in_ref, in_all)

    def owner_of(j):
        return n_rep // 2 - 1 + j % 2

    def has_away(j):
        o = owner_of(j)
        return jnp.logical_or(
            jnp.logical_and(me_r < o, me_r > 0),
            jnp.logical_and(me_r > o, me_r < n_rep - 1),
        )

    def partial_copy(j):
        o = owner_of(j)
        side = jnp.where(me_r < o, 0, 1)
        toward = jnp.clip(jnp.where(me_r < o, me_r + 1, me_r - 1), 0, n_rep - 1)
        return remote(
            stage.at[j], part.at[side, j], part_send.at[j], part_recv.at[side, j], {"rep": toward}
        )

    def wait_part(side, j):
        remote(
            stage.at[j], part.at[side, j], part_send.at[j], part_recv.at[side, j], {"rep": me_r}
        ).wait_recv()

    def spot(j):
        return j // per_grad, pl.ds(0, ff), pl.ds(j % per_grad * CHUNK, CHUNK)

    def final_copy(j, way):
        target = jnp.clip(me_r + (1 if way else -1), 0, n_rep - 1)
        return remote(
            land.at[j], land.at[j], fin_send.at[way, j], fin_recv.at[j], {"rep": target}
        )

    def is_edge(j):
        return jnp.logical_and(me_r != owner_of(j), jnp.logical_not(has_away(j)))

    def start_edge(j):
        @pl.when(is_edge(j))
        def _():
            partial_copy(j).start()

    def refill(j):
        if j + FLIGHT < chunks:

            @pl.when(is_edge(j))
            def _():
                partial_copy(j).wait_send()
                partial_copy(j + FLIGHT).start()

    def pass_on(j):
        o = owner_of(j)
        for side in (0, 1):
            inner = (me_r < o) if side == 0 else (me_r > o)

            @pl.when(jnp.logical_and(inner, has_away(j)))
            def _(side=side):
                wait_part(side, j)
                stage[j] = (stage[j].astype(F32) + part[side, j].astype(F32)).astype(BF16)
                partial_copy(j).start()

    def own_sum(j):
        o = owner_of(j)

        @pl.when(me_r == o)
        def _():
            total = stage[j].astype(F32)
            if o > 0:
                wait_part(0, j)
                total = total + part[0, j].astype(F32)
            if o < n_rep - 1:
                wait_part(1, j)
                total = total + part[1, j].astype(F32)
            land[j] = total.astype(BF16)
            if o > 0:
                final_copy(j, 0).start()
            if o < n_rep - 1:
                final_copy(j, 1).start()

    def deliver(j):
        o = owner_of(j)

        @pl.when(me_r != o)
        def _():
            final_copy(j, 0).wait_recv()

        @pl.when(jnp.logical_and(me_r < o, me_r > 0))
        def _():
            final_copy(j, 0).start()

        @pl.when(jnp.logical_and(me_r > o, me_r < n_rep - 1))
        def _():
            final_copy(j, 1).start()

    def settle(j):
        deliver(j)
        fin[spot(j)] = land[j]

    def advance(k, fill=True):
        if k < chunks:
            if fill:
                refill(k)
            pass_on(k)
        if 0 <= k - OWN_LAG < chunks:
            own_sum(k - OWN_LAG)
        if 0 <= k - LAG < chunks:
            settle(k - LAG)

    over_rows = (((0,), (0,)), ((), ()))
    over_cols = (((1,), (1,)), ((), ()))

    def weight_grad(grad, left, right):
        for piece in range(width // WIDE):
            product = jnp.dot(
                left[...], right[:, pl.ds(piece * WIDE, WIDE)], preferred_element_type=F32
            ).astype(BF16)
            for sub in range(WIDE // CHUNK):
                j = grad * per_grad + piece * (WIDE // CHUNK) + sub
                stage[j] = product[:, sub * CHUNK : (sub + 1) * CHUNK]
                if j < FLIGHT:
                    start_edge(j)

    weight_grad(0, hid, cot_all)

    for piece in range(seq // WIDE):
        cols = pl.ds(piece * WIDE, WIDE)
        d_hid[:, cols] = lax.dot_general(
            down_b[...], cot_all[cols, :], over_cols, preferred_element_type=F32
        ).astype(BF16)
    advance(0, False)

    def backward(at, _):
        rows = pl.ds(pl.multiple_of(at * ROWS, ROWS), ROWS)
        d_hidden = d_hid[rows, :].astype(F32)
        dgate[rows, :] = (d_hidden * act[rows, :]).astype(BF16)
        d_conv = d_hidden * slope_gate[rows, :]
        up = up_raw[rows, :].astype(F32)
        total = jnp.zeros((ROWS, seq), F32)
        for k in range(taps):
            ahead = sooner(d_conv, k)
            total = total + in_cols[rows, k : k + 1] * ahead
            in_cols[rows, taps + 1 + k : taps + 2 + k] = jnp.sum(ahead * up, axis=1, keepdims=True)
        in_cols[rows, 2 * taps + 1 : 2 * taps + 2] = jnp.sum(d_conv, axis=1, keepdims=True)
        dup[rows, :] = total.astype(BF16)
        return 0

    lax.fori_loop(0, ff // ROWS, backward, 0)
    in_rows[...] = in_cols[...].T
    conv_all[me_r] = in_rows[pl.ds(0, 8), :]

    for step in range(1, n_rep):
        copy = remote(
            conv_all.at[me_r],
            conv_all.at[me_r],
            conv_send.at[step],
            conv_recv.at[me_r],
            {"rep": other(me_r, step, n_rep)},
        )
        copy.start()
        pending.append(copy)

    advance(1, False)
    pending += gather_finish(1, in_ref, in_all)
    weight_grad(1, dup, in_all)
    for j in range(2):
        refill(j)
    advance(2)
    weight_grad(2, dgate, in_all)
    advance(3)

    def input_rows(core, store):
        left_up = jnp.concatenate(
            [dup[:, rows_of(f * n_tp + core)] for f in range(n_fs)], axis=1
        )
        left_gate = jnp.concatenate(
            [dgate[:, rows_of(f * n_tp + core)] for f in range(n_fs)], axis=1
        )
        for piece in range(width // WIDE):
            cols = pl.ds(piece * WIDE, WIDE)
            total = lax.dot_general(
                left_up, up_b[:, cols], over_rows, preferred_element_type=F32
            ) + lax.dot_general(
                left_gate, gate_b[:, cols], over_rows, preferred_element_type=F32
            )
            store(cols, total)

    for hop in range(1, n_tp):

        def store_pair(cols, total, hop=hop):
            pair_send[hop - 1, :, cols] = total.astype(BF16)

        input_rows(other(me_c, hop, n_tp), store_pair)
        copy = remote(
            pair_send.at[hop - 1],
            pair_recv.at[hop - 1],
            pair_ssem.at[hop - 1],
            pair_rsem.at[hop - 1],
            {"tp": other(me_c, hop, n_tp)},
        )
        copy.start()
        pending.append(copy)
    advance(4)

    def store_keep(cols, total):
        keep[:, cols] = total

    input_rows(me_c, store_keep)
    for hop in range(1, n_tp):
        remote(
            pair_send.at[hop - 1],
            pair_recv.at[hop - 1],
            pair_ssem.at[hop - 1],
            pair_rsem.at[hop - 1],
            {"tp": other(me_c, hop, n_tp)},
        ).wait_recv()
    for step in range(1, n_fs):
        target = other(me_f, step, n_fs)
        rows = rows_of(target)
        total = keep[rows, :]
        for hop in range(1, n_tp):
            total = total + pair_recv[hop - 1, rows, :].astype(F32)
        ring_send[step] = total.astype(BF16)
        copy = remote(
            ring_send.at[step],
            ring_recv.at[step],
            ring_ssem.at[step],
            ring_rsem.at[step],
            {"fs": target},
        )
        copy.start()
        pending.append(copy)
    for j in range(5, chunks):
        advance(j)

    own = rows_of(me_f)
    total = keep[own, :]
    for hop in range(1, n_tp):
        total = total + pair_recv[hop - 1, own, :].astype(F32)
    for step in range(1, n_fs):
        remote(
            ring_send.at[step],
            ring_recv.at[step],
            ring_ssem.at[step],
            ring_rsem.at[step],
            {"fs": me_f},
        ).wait_recv()
        total = total + ring_recv[step].astype(F32)
    gi_ref[...] = total.astype(BF16)

    for step in range(1, n_rep):
        source = other(me_r, n_rep - step, n_rep)
        remote(
            conv_all.at[source],
            conv_all.at[source],
            conv_send.at[0],
            conv_recv.at[source],
            {"rep": me_r},
        ).wait_recv()
    total = conv_all[0]
    for at in range(1, n_rep):
        total = total + conv_all[at]
    taps_out[...] = total[taps + 1 : 2 * taps + 1, :ff] * factor
    bias_out[...] = total[2 * taps + 1 : 2 * taps + 2, :ff] * factor

    for j in range(chunks, chunks + LAG):
        advance(j)

    for copy in pending:
        copy.wait_send()
    for j in range(chunks):
        o = owner_of(j)

        unsent = me_r != o
        if j + FLIGHT < chunks:
            unsent = jnp.logical_and(unsent, has_away(j))

        @pl.when(unsent)
        def _():
            partial_copy(j).wait_send()

        @pl.when(jnp.logical_and(me_r <= o, me_r > 0))
        def _():
            final_copy(j, 0).wait_send()

        @pl.when(jnp.logical_and(me_r >= o, me_r < n_rep - 1))
        def _():
            final_copy(j, 1).wait_send()


def on_device(
    sizes, inputs, up_pre, gate_pre, cotangent, w_up, w_gate, w_down, conv_weight, conv_bias
):
    n_rep, n_fs, n_tp = sizes
    seq, ff = up_pre.shape[1:]
    block, width = inputs.shape[1:]
    taps = conv_weight.shape[0]
    factor = float(n_rep * seq) ** (-0.5)
    chunks = 3 * width // CHUNK
    devices = n_fs * n_tp
    vmem = pl.BlockSpec(memory_space=pltpu.VMEM)
    hbm = pl.BlockSpec(memory_space=pl.ANY)
    dma = pltpu.SemaphoreType.DMA
    padded = -(-ff // LANES) * LANES
    grad_inputs, fin, g_taps, g_bias = pl.pallas_call(
        functools.partial(kernel, sizes),
        out_shape=(
            jax.ShapeDtypeStruct((block, width), BF16),
            jax.ShapeDtypeStruct((3, ff, width), BF16),
            jax.ShapeDtypeStruct((taps, ff), F32),
            jax.ShapeDtypeStruct((1, ff), F32),
        ),
        in_specs=[vmem] * 4 + [hbm] * 5,
        out_specs=(vmem,) * 4,
        scratch_shapes=[
            pltpu.VMEM((seq, width), BF16),
            pltpu.VMEM((seq, width), BF16),
            pltpu.VMEM((ff, seq), BF16),
            pltpu.VMEM((ff, seq), BF16),
            pltpu.VMEM((ff, width), F32),
            pltpu.VMEM((ff, width), F32),
            pltpu.VMEM((ff, width), F32),
            pltpu.VMEM((ff, seq), F32),
            pltpu.VMEM((ff, seq), F32),
            pltpu.VMEM((ff, seq), BF16),
            pltpu.VMEM((ff, seq), BF16),
            pltpu.VMEM((ff, seq), BF16),
            pltpu.VMEM((ff, seq), BF16),
            pltpu.VMEM((ff, width), BF16),
            pltpu.VMEM((ff, width), BF16),
            pltpu.VMEM((ff, width), BF16),
            pltpu.VMEM((LANES, padded), F32),
            pltpu.VMEM((padded, LANES), F32),
            pltpu.VMEM((2, chunks, ff, CHUNK), BF16),
            pltpu.VMEM((chunks, ff, CHUNK), BF16),
            pltpu.VMEM((chunks, ff, CHUNK), BF16),
            pltpu.VMEM((n_rep, 8, padded), F32),
            pltpu.VMEM((n_tp - 1, n_fs * block, width), BF16),
            pltpu.VMEM((n_tp - 1, n_fs * block, width), BF16),
            pltpu.VMEM((n_fs * block, width), F32),
            pltpu.VMEM((n_fs, block, width), BF16),
            pltpu.VMEM((n_fs, block, width), BF16),
            dma((5,)),
            dma((2, n_fs * n_tp)),
            dma((2, devices)),
            dma((chunks,)),
            dma((2, chunks)),
            dma((2, chunks)),
            dma((chunks,)),
            dma((n_rep,)),
            dma((n_rep,)),
            dma((n_tp,)),
            dma((n_tp,)),
            dma((n_fs,)),
            dma((n_fs,)),
        ],
        compiler_params=pltpu.CompilerParams(
            collective_id=0, has_side_effects=True, vmem_limit_bytes=62 << 20
        ),
    )(
        cotangent[0],
        inputs[0],
        conv_weight,
        conv_bias[None],
        up_pre[0].T,
        gate_pre[0].T,
        w_down,
        w_up.T,
        w_gate.T,
    )
    g_down = fin[0].astype(F32) * factor
    g_up = fin[1].T.astype(F32) * factor
    g_gate = fin[2].T.astype(F32) * factor
    return grad_inputs[None], g_up, g_gate, g_down, g_taps, g_bias[0]


def solution(mesh):
    sizes = tuple(mesh.shape[axis] for axis in ("rep", "fs", "tp"))
    return jax.shard_map(
        functools.partial(on_device, sizes),
        mesh=mesh,
        in_specs=(
            P("rep", ("fs", "tp"), None),
            P("rep", None, ("fs", "tp")),
            P("rep", None, ("fs", "tp")),
            P("rep", ("fs", "tp"), None),
            P(None, ("fs", "tp")),
            P(None, ("fs", "tp")),
            P(("fs", "tp"), None),
            P(None, ("fs", "tp")),
            P(("fs", "tp")),
        ),
        out_specs=(
            P("rep", ("fs", "tp"), None),
            P(None, ("fs", "tp")),
            P(None, ("fs", "tp")),
            P(("fs", "tp"), None),
            P(None, ("fs", "tp")),
            P(("fs", "tp")),
        ),
        check_vma=False,
    )
```
